32 devices in a mesh: sp: 8 (over z, y), tp: 4 (over x, core).
Axes of the slice: x: 2, y: 2, z: 4, core: 2. Of those that a mesh axis runs over, the one named last changes fastest.
Arguments:
- residual: bfloat16 [8192, 2048], P('sp'), may hold values from -6 to 6
- small_heads: bfloat16 [8192, 1024], P('sp', 'tp'), may hold values from -6 to 6
- large_heads: bfloat16 [8192, 1024], P('sp', 'tp'), may hold values from -6 to 6
- state_keys: bfloat16 [8192, 8, 128], P('sp', 'tp'), may hold values from -6 to 6
- state_queries: bfloat16 [8192, 8, 128], P('sp', 'tp'), may hold values from -6 to 6
- small_gate: bfloat16 [8192, 1024], P('sp', 'tp'), may hold values from -6 to 6
- large_gate: bfloat16 [8192, 1024], P('sp', 'tp'), may hold values from -6 to 6
- small_step: float32 [8192, 16], P('sp', 'tp'), may hold values from -3 to 2
- large_step: float32 [8192, 8], P('sp', 'tp'), may hold values from -3 to 2
- small_taps: bfloat16 [4, 1024], P(None, 'tp'), may hold values from -3 to 3
- large_taps: bfloat16 [4, 1024], P(None, 'tp'), may hold values from -3 to 3
- key_taps: bfloat16 [4, 8, 128], P(None, 'tp'), may hold values from -3 to 3
- query_taps: bfloat16 [4, 8, 128], P(None, 'tp'), may hold values from -3 to 3
- small_decay: float32 [16], P('tp'), may hold values from -12 to -2, as said below
- large_decay: float32 [8], P('tp'), may hold values from -12 to -2, as said below
- small_gain: bfloat16 [1024], P('tp'), may hold values from 0.099609375 to 1.8984375
- large_gain: bfloat16 [1024], P('tp'), may hold values from 0.099609375 to 1.8984375
- small_out: bfloat16 [1024, 2048], P('tp'), may hold values from -0.125 to 0.125
- large_out: bfloat16 [1024, 2048], P('tp'), may hold values from -0.125 to 0.125
- mixer_gain: bfloat16 [2048], replicated, may hold values from 0.099609375 to 1.8984375
- ffn_in_gain: bfloat16 [2048], replicated, may hold values from 0.099609375 to 1.8984375
- gate_proj: bfloat16 [2048, 5632], P('sp', 'tp'), may hold values from -0.125 to 0.125
- up_proj: bfloat16 [2048, 5632], P('sp', 'tp'), may hold values from -0.125 to 0.125
- down_proj: bfloat16 [2048, 5632], P('sp', 'tp'), may hold values from -0.078125 to 0.078125
- ffn_out_gain: bfloat16 [2048], replicated, may hold values from 0.099609375 to 1.8984375
Outputs:
- updated: bfloat16 [8192, 2048], P(('sp', 'tp'))
The draws below stay inside these ranges and needn't reach their ends.
Inputs may be any that keep to these rules, and one draw needn't show every extreme that they name: `small_decay`: log decay rates of the first group. `large_decay`: log decay rates of the second group.
All inputs are finite; a program needn't handle non-finite values.
Results may differ from the reference program's by a relative error of at most 0.014.
Values may be sent and summed in bfloat16 or wider, within the bound.
A program may use at most 192 MiB of HBM per device.

```python
import jax
import jax.numpy as jnp
from jax import lax

D = 2048
FF = 5632
HA = 16
PA = 64
HB = 8
PB = 128
GROUPS = 8
STATE = 128
CONV = 4
BLOCK = 128
TOK_DEV = 1024
TOKENS = 8192
HEAD_BLOCKS = 4


def step_law(key, heads, salt):
    rows = jnp.arange(TOKENS, dtype=jnp.int32) // TOK_DEV
    offset_key = jax.random.fold_in(key, 101)
    jitter_key = jax.random.fold_in(key, salt)
    offsets = jax.random.uniform(offset_key, (TOKENS // TOK_DEV,), jnp.float32, -1.5, 0.5)
    jitter = jnp.clip(0.5 * jax.random.normal(jitter_key, (TOKENS, heads), jnp.float32), -1.5, 1.5)
    return offsets[rows][:, None] + jitter


def decay_law(key, heads, salt):
    base_key = jax.random.fold_in(key, salt)
    order_key, slow_key, fast_key = jax.random.split(base_key, 3)
    fast_count = heads // 2
    ranks = jax.random.permutation(order_key, heads)
    slow_values = jnp.log(jax.random.uniform(slow_key, (heads,), jnp.float32, 0.25, 1.5) / TOKENS)
    fast_values = jnp.log(jax.random.uniform(fast_key, (heads,), jnp.float32, 1.0 / 60.0, 1.0 / 20.0))
    return jnp.where(ranks < fast_count, fast_values, slow_values)


def draw_small_step(key, part):
    return step_law(key, HA, 11)


def draw_large_step(key, part):
    return step_law(key, HB, 12)


def draw_small_decay(key, part):
    return decay_law(key, HA, 21)


def draw_large_decay(key, part):
    return decay_law(key, HB, 22)


def shard_levels(rng, shape, pieces, low, top_value):
    def one(position, parts):
        draws = jax.random.uniform(jax.random.fold_in(jax.random.fold_in(rng, 6), position), (parts,), jnp.float32, low / len(pieces), top_value / len(pieces))
        return jnp.repeat(jnp.exp(draws), shape[position] // parts).reshape((-1,) + (1,) * (len(shape) - position - 1))

    loudness = one(*pieces[0])
    for cut in pieces[1:]:
        loudness = loudness * one(*cut)
    return loudness


def scatter_about(rng, shape, width, bound, cuts=(), kind=jnp.bfloat16):
    level = shard_levels(rng, shape, cuts, -0.22, 0.18) if cuts else 1.0
    drawn = jax.random.normal(rng, shape, jnp.float32) * width * level
    return jnp.minimum(jnp.maximum(drawn, -bound), bound).astype(kind)


def setup_inputs(seed: int = 0) -> dict:
    arg_keys = jax.random.split(jax.random.key(seed), 26)
    return {
        "residual": scatter_about(arg_keys[0], (TOKENS, D), 1.0, 6.0, ((0, 8),)),
        "small_heads": scatter_about(arg_keys[1], (TOKENS, HA * PA), 1.0, 6.0, ((0, 8), (1, 4))),
        "large_heads": scatter_about(arg_keys[2], (TOKENS, HB * PB), 1.0, 6.0, ((0, 8), (1, 4))),
        "state_keys": scatter_about(arg_keys[3], (TOKENS, GROUPS, STATE), 1.0, 6.0, ((0, 8), (1, 4))),
        "state_queries": scatter_about(arg_keys[4], (TOKENS, GROUPS, STATE), 1.0, 6.0, ((0, 8), (1, 4))),
        "small_gate": scatter_about(arg_keys[5], (TOKENS, HA * PA), 1.0, 6.0, ((0, 8), (1, 4))),
        "large_gate": scatter_about(arg_keys[6], (TOKENS, HB * PB), 1.0, 6.0, ((0, 8), (1, 4))),
        "small_step": draw_small_step(jax.random.fold_in(arg_keys[25], 71), 0),
        "large_step": draw_large_step(jax.random.fold_in(arg_keys[25], 71), 0),
        "small_taps": scatter_about(arg_keys[9], (CONV, HA * PA), CONV ** -0.5, 3.0, ((1, 4),)),
        "large_taps": scatter_about(arg_keys[10], (CONV, HB * PB), CONV ** -0.5, 3.0, ((1, 4),)),
        "key_taps": scatter_about(arg_keys[11], (CONV, GROUPS, STATE), CONV ** -0.5, 3.0, ((1, 4),)),
        "query_taps": scatter_about(arg_keys[12], (CONV, GROUPS, STATE), CONV ** -0.5, 3.0, ((1, 4),)),
        "small_decay": draw_small_decay(jax.random.fold_in(arg_keys[25], 71), 0),
        "large_decay": draw_large_decay(jax.random.fold_in(arg_keys[25], 71), 0),
        "small_gain": jnp.clip(1.0 + 0.18 * jax.random.normal(arg_keys[15], (HA * PA,), jnp.float32), 0.099609375, 1.8984375).astype(jnp.bfloat16),
        "large_gain": jnp.clip(1.0 + 0.18 * jax.random.normal(arg_keys[16], (HB * PB,), jnp.float32), 0.099609375, 1.8984375).astype(jnp.bfloat16),
        "small_out": scatter_about(arg_keys[17], (HA * PA, D), (HA * PA + HB * PB) ** -0.5, 0.125, ((0, 4),)),
        "large_out": scatter_about(arg_keys[18], (HB * PB, D), (HA * PA + HB * PB) ** -0.5, 0.125, ((0, 4),)),
        "mixer_gain": jnp.clip(1.0 + 0.18 * jax.random.normal(arg_keys[19], (D,), jnp.float32), 0.099609375, 1.8984375).astype(jnp.bfloat16),
        "ffn_in_gain": jnp.clip(1.0 + 0.18 * jax.random.normal(arg_keys[20], (D,), jnp.float32), 0.099609375, 1.8984375).astype(jnp.bfloat16),
        "gate_proj": scatter_about(arg_keys[21], (D, FF), D ** -0.5, 0.125, ((0, 8), (1, 4))),
        "up_proj": scatter_about(arg_keys[22], (D, FF), D ** -0.5, 0.125, ((0, 8), (1, 4))),
        "down_proj": scatter_about(arg_keys[23], (D, FF), FF ** -0.5, 0.078125, ((0, 8), (1, 4))),
        "ffn_out_gain": jnp.clip(1.0 + 0.18 * jax.random.normal(arg_keys[24], (D,), jnp.float32), 0.099609375, 1.8984375).astype(jnp.bfloat16),
    }


EPS = 1e-06

def rounded(values):
    return lax.optimization_barrier(values.astype(jnp.bfloat16)).astype(jnp.float32)

def causal_taps(extended, tap_weights, length):
    kernel_len = tap_weights.shape[0]
    summed = jnp.zeros((length,) + extended.shape[1:], jnp.float32)
    for offset in range(kernel_len):
        window_rows = extended[offset:offset + length].astype(jnp.float32)
        summed = summed + tap_weights[offset].astype(jnp.float32) * window_rows
    return jax.nn.silu(summed).astype(jnp.bfloat16)

def block_pass(values, key_rows, queries, step_sizes, decay_rates):
    length, groups, head_count, head_dim = values.shape
    block_count = length // BLOCK
    state_len = key_rows.shape[-1]
    log_decay = -step_sizes * decay_rates
    causal = jnp.tril(jnp.ones((BLOCK, BLOCK), dtype=bool))
    highest = lax.Precision.HIGHEST

    def one_block(carry_state, block):
        block_values, block_keys, block_queries, block_steps, block_decay = block
        values_wide = block_values.astype(jnp.float32)
        keys_wide = block_keys.astype(jnp.float32)
        queries_wide = block_queries.astype(jnp.float32)
        cumulative = jnp.cumsum(block_decay, axis=0)
        scores = jnp.einsum('lgn,sgn->gls', queries_wide, keys_wide, precision=highest)
        cum_heads = jnp.transpose(cumulative, (1, 2, 0))
        gap_matrix = cum_heads[:, :, :, None] - cum_heads[:, :, None, :]
        decays = jnp.exp(jnp.where(causal, gap_matrix, -jnp.inf))
        step_heads = jnp.transpose(block_steps, (1, 2, 0))[:, :, None, :]
        weights = rounded(scores[:, None] * decays * step_heads)
        inside = jnp.einsum('ghls,sghp->lghp', weights, values_wide, precision=highest)
        carried = jnp.einsum('lgn,ghpn->lghp', queries_wide, carry_state, precision=highest)
        carried = carried * jnp.exp(cumulative)[..., None]
        tail_sum = cumulative[-1]
        scaled = rounded(values_wide * (block_steps * jnp.exp(tail_sum - cumulative))[..., None])
        fresh_state = jnp.einsum('lghp,lgn->ghpn', scaled, keys_wide, precision=highest)
        next_state = carry_state * jnp.exp(tail_sum)[..., None, None] + fresh_state
        return (next_state, inside + carried)
    blocked = (values.reshape(block_count, BLOCK, groups, head_count, head_dim), key_rows.reshape(block_count, BLOCK, groups, state_len), queries.reshape(block_count, BLOCK, groups, state_len), step_sizes.reshape(block_count, BLOCK, groups, head_count), log_decay.reshape(block_count, BLOCK, groups, head_count))
    start_state = jnp.zeros((groups, head_count, head_dim, state_len), jnp.float32)
    end_state, outputs = lax.scan(one_block, start_state, blocked)
    return outputs.reshape(length, groups, head_count, head_dim)

def head_group(values, key_rows, queries, step_raw, decay_log):
    length = values.shape[0]
    head_count = step_raw.shape[1]
    groups = key_rows.shape[1]
    per_group = head_count // groups
    head_dim = values.shape[1] // head_count
    step_sizes = jax.nn.softplus(step_raw.astype(jnp.float32)).reshape(length, groups, per_group)
    decay_rates = jnp.exp(decay_log.astype(jnp.float32)).reshape(groups, per_group)
    return block_pass(values.reshape(length, groups, per_group, head_dim), key_rows, queries, step_sizes, decay_rates)

def unit_rms(values):
    return values * lax.rsqrt(lax.optimization_barrier(jnp.mean(values * values, axis=-1, keepdims=True)) + EPS)

def gate_and_norm(mixed_heads, gate_raw, gain):
    length, groups, per_group, head_dim = mixed_heads.shape
    gated = mixed_heads.reshape(length, -1) * jax.nn.silu(gate_raw.astype(jnp.float32))
    normed = unit_rms(gated.reshape(length, groups * per_group, head_dim))
    return (normed.reshape(length, -1) * gain.astype(jnp.float32)).astype(jnp.bfloat16)

def blockwise_sum(pairs, length, features):
    summed = jnp.zeros((length, features), jnp.float32)
    for index in range(HEAD_BLOCKS):
        partial_value = jnp.zeros((length, features), jnp.float32)
        for left, right in pairs:
            cols = left.shape[1] // HEAD_BLOCKS
            partial_value = partial_value + jnp.dot(left[:, index * cols:(index + 1) * cols], right[index * cols:(index + 1) * cols], preferred_element_type=jnp.float32)
        summed = summed + rounded(partial_value)
    return summed

def reference(residual, small_heads, large_heads, state_keys, state_queries, small_gate, large_gate, small_step, large_step, small_taps, large_taps, key_taps, query_taps, small_decay, large_decay, small_gain, large_gain, small_out, large_out, mixer_gain, ffn_in_gain, gate_proj, up_proj, down_proj, ffn_out_gain):
    length = residual.shape[0]
    halo_rows = small_taps.shape[0] - 1

    def extended(values):
        return jnp.concatenate([jnp.zeros((halo_rows,) + values.shape[1:], values.dtype), values], axis=0)
    small_conv = causal_taps(extended(small_heads), small_taps, length)
    large_conv = causal_taps(extended(large_heads), large_taps, length)
    key_conv = causal_taps(extended(state_keys), key_taps, length)
    query_conv = causal_taps(extended(state_queries), query_taps, length)
    small_mix = head_group(small_conv, key_conv[:, 0::2], query_conv[:, 0::2], small_step, small_decay)
    large_mix = head_group(large_conv, key_conv[:, 1::2], query_conv[:, 1::2], large_step, large_decay)
    small_normed = gate_and_norm(small_mix, small_gate, small_gain)
    large_normed = gate_and_norm(large_mix, large_gate, large_gain)
    mix = blockwise_sum([(small_normed, small_out), (large_normed, large_out)], length, D)
    mixed = residual.astype(jnp.float32) + unit_rms(mix) * mixer_gain.astype(jnp.float32)
    normed_in = (unit_rms(mixed) * ffn_in_gain.astype(jnp.float32)).astype(jnp.bfloat16)
    gate = jnp.dot(normed_in, gate_proj, preferred_element_type=jnp.float32)
    up_values = jnp.dot(normed_in, up_proj, preferred_element_type=jnp.float32)
    hidden = (jax.nn.silu(gate) * up_values).astype(jnp.bfloat16)
    ffn = blockwise_sum([(hidden, jnp.transpose(down_proj))], length, D)
    updated = mixed + 0.5 * unit_rms(ffn) * ffn_out_gain.astype(jnp.float32)
    return updated.astype(jnp.bfloat16)
```

```python
import functools

import jax
import jax.numpy as jnp
from jax import lax
from jax.experimental import pallas as pl
from jax.experimental.pallas import tpu as pltpu
from jax.sharding import PartitionSpec as P

BLOCK = 128
HALO = 16
LANES = 128
SLOTS = 8
TAIL = 16


EPS = 1e-06
FAR = -1e30
F32 = jnp.float32
BF16 = jnp.bfloat16


def moved(block, axis, route):
    return lax.ppermute(block, axis, route)


def earlier(block, axis, distance):
    devices = range(lax.axis_size(axis))
    return moved(block, axis, [(i - distance, i) for i in devices if i - distance in devices])


def paired(block, axis, bit):
    return moved(block, axis, [(i, i ^ bit) for i in range(lax.axis_size(axis))])


def silu(x):
    return x / (1.0 + jnp.exp(-x))


def softplus(x):
    return jnp.maximum(x, 0.0) + jnp.log1p(jnp.exp(-jnp.abs(x)))


def exact_dot(a, b):
    return lax.dot_general(
        a, b, (((1,), (0,)), ((), ())), precision=lax.Precision.HIGHEST, preferred_element_type=F32
    )


def lower(n):
    rows = lax.broadcasted_iota(jnp.int32, (n, n), 0)
    return rows >= lax.broadcasted_iota(jnp.int32, (n, n), 1)


def spread(columns, heads, dim):
    rows = columns.shape[0]
    parts = []
    if dim >= LANES:
        for h in heads:
            parts.append(jnp.broadcast_to(columns[:, h : h + 1], (rows, dim)))
    else:
        per = LANES // dim
        lane = lax.broadcasted_iota(jnp.int32, (rows, LANES), 1)
        for first in range(0, len(heads), per):
            part = jnp.broadcast_to(columns[:, heads[first] : heads[first] + 1], (rows, LANES))
            for j in range(1, per):
                h = heads[first + j]
                part = jnp.where(lane >= j * dim, columns[:, h : h + 1], part)
            parts.append(part)
    return jnp.concatenate(parts, axis=1)


def conv_kernel(
    sizes, small, large, keys, queries, halo, taps, steps, decay, conv, packed, before, state, total
):
    (heads_a, dim_a), (heads_b, dim_b), state_len = sizes
    step = pl.program_id(0)

    @pl.when(step == 0)
    def _():
        before[...] = halo[...]
        state[...] = jnp.zeros_like(state)
        total[...] = jnp.zeros_like(total)

    column = 0
    pieces = []
    for ref in (small, large, keys, queries):
        width = ref.shape[1]
        for start in range(0, width, LANES):
            here = pl.ds(column, LANES)
            now = ref[:, pl.ds(start, LANES)]
            extended = jnp.concatenate([before[:, here], now], axis=0).astype(F32)
            kernel_len = taps.shape[0]
            summed = None
            for k in range(kernel_len):
                first = HALO - kernel_len + 1 + k
                term = taps[k : k + 1, here] * extended[first : first + BLOCK]
                summed = term if summed is None else summed + term
            done = silu(summed).astype(BF16)
            conv[:, here] = done
            before[:, here] = now[BLOCK - HALO :]
            pieces.append(done)
            column += LANES
    dt = softplus(steps[...])
    cum = exact_dot(lower(BLOCK).astype(F32), -dt * jnp.exp(decay[...]))
    tail = cum[BLOCK - 1 : BLOCK]
    scale = dt * jnp.exp(tail - cum)
    head_list_a = list(range(heads_a))
    head_list_b = list(range(heads_a, heads_a + heads_b))
    kept = jnp.exp(tail)
    offset = 0
    width_a = heads_a * dim_a
    width_b = heads_b * dim_b
    for heads, dim, width, key_at in (
        (head_list_a, dim_a, width_a, width_a + width_b),
        (head_list_b, dim_b, width_b, width_a + width_b + state_len),
    ):
        x = conv[:, offset : offset + width].astype(F32)
        u = (x * spread(scale, heads, dim)).astype(BF16)
        k = conv[:, key_at : key_at + state_len]
        fresh = lax.dot_general(k, u, (((0,), (0,)), ((), ())), preferred_element_type=F32)
        old = state[:, offset : offset + width]
        state[:, offset : offset + width] = old * spread(kept, heads, dim) + fresh
        offset += width
    total[...] = total[...] + tail

    @pl.when(step == pl.num_programs(0) - 1)
    def _():
        packed[:state_len] = state[...].astype(BF16)
        whole = jnp.concatenate(
            [spread(total[...], head_list_a, dim_a), spread(total[...], head_list_b, dim_b)], axis=1
        )
        high = whole.astype(BF16)
        low = (whole - high.astype(F32)).astype(BF16)
        row = lax.broadcasted_iota(jnp.int32, (TAIL, whole.shape[1]), 0)
        both = jnp.where(row == 0, high.astype(F32), jnp.where(row == 1, low.astype(F32), 0.0))
        packed[state_len:] = both.astype(BF16)


def mix_kernel(
    sizes,
    place,
    conv,
    small_gate,
    large_gate,
    steps,
    steps_across,
    decay,
    decay_across,
    gain,
    small_out,
    large_out,
    entering,
    partial_out,
    state,
):
    (heads_a, dim_a), (heads_b, dim_b), state_len = sizes
    step = pl.program_id(0)

    @pl.when(step == 0)
    def _():
        state[...] = entering[...]

    causal = lower(BLOCK)
    ones = causal.astype(F32)
    dt = softplus(steps[...])
    cum = exact_dot(ones, -dt * jnp.exp(decay[...]))
    dt_across = softplus(steps_across[...])
    upper = (
        lax.broadcasted_iota(jnp.int32, (BLOCK, BLOCK), 0)
        <= lax.broadcasted_iota(jnp.int32, (BLOCK, BLOCK), 1)
    ).astype(F32)
    cum_across = exact_dot(-dt_across * jnp.exp(decay_across[...]), upper)
    tail = cum[BLOCK - 1 : BLOCK]
    scale = dt * jnp.exp(tail - cum)
    grown = jnp.exp(cum)
    kept = jnp.exp(tail)
    width_a = heads_a * dim_a
    width_b = heads_b * dim_b
    offset = 0
    result = None
    lane = lax.broadcasted_iota(jnp.int32, (BLOCK, LANES), 1)
    for which, (heads, dim, width, gate, out) in enumerate(
        (
            (list(range(heads_a)), dim_a, width_a, small_gate, small_out),
            (list(range(heads_a, heads_a + heads_b)), dim_b, width_b, large_gate, large_out),
        )
    ):
        key_at = width_a + width_b + which * state_len
        query_at = key_at + 2 * state_len
        x = conv[:, offset : offset + width]
        k = conv[:, key_at : key_at + state_len]
        q = conv[:, query_at : query_at + state_len]
        scores = lax.dot_general(q, k, (((1,), (1,)), ((), ())), preferred_element_type=F32)
        old = state[:, offset : offset + width]
        carried = jnp.dot(q, old.astype(BF16), preferred_element_type=F32)
        carried = carried * spread(grown, heads, dim)
        u = (x.astype(F32) * spread(scale, heads, dim)).astype(BF16)
        fresh = lax.dot_general(k, u, (((0,), (0,)), ((), ())), preferred_element_type=F32)
        state[:, offset : offset + width] = old * spread(kept, heads, dim) + fresh
        inside = []
        span = max(dim, LANES)
        per = span // dim
        for first in range(0, len(heads), per):
            x_part = x[:, first * dim : first * dim + span]
            part = None
            for j in range(per):
                h = heads[first + j]
                gap = cum[:, h : h + 1] - cum_across[h : h + 1]
                decays = jnp.exp(jnp.where(causal, gap, FAR))
                w = (scores * decays * dt_across[h : h + 1]).astype(BF16)
                got = jnp.dot(w, x_part, preferred_element_type=F32)
                part = got if part is None else jnp.where(lane >= j * dim, got, part)
            inside.append(part)
        mixed = jnp.concatenate(inside, axis=1) + carried
        gated = mixed * silu(gate[...].astype(F32))
        squares = gated * gated
        normed = []
        for first in range(0, len(heads), per):
            at = first * dim
            part = squares[:, at : at + span]
            means = None
            for j in range(per):
                if per == 1:
                    means = jnp.sum(part, axis=1, keepdims=True)
                else:
                    ours = (lane >= j * dim) & (lane < (j + 1) * dim)
                    one = jnp.sum(jnp.where(ours, part, 0.0), axis=1, keepdims=True)
                    means = one if means is None else jnp.where(lane >= j * dim, one, means)
            normed.append(gated[:, at : at + span] * lax.rsqrt(means * (1.0 / dim) + EPS))
        normed = jnp.concatenate(normed, axis=1) * gain[:, offset : offset + width]
        product = jnp.dot(normed.astype(BF16), out[...], preferred_element_type=F32)
        result = product if result is None else result + product
        offset += width
    partial_out[...] = result.astype(BF16)[None]


def unit_rms(values):
    return values * lax.rsqrt(jnp.mean(values * values, axis=-1, keepdims=True) + EPS)


def reversed_bits(value, count):
    out = 0
    bit = 1
    while bit < count:
        out = out * 2 + (value // bit) % 2
        bit *= 2
    return out


def scattered(blocks, axis):
    bit = 1
    while blocks.shape[0] > 1:
        half = blocks.shape[0] // 2
        other = paired(blocks[half:], axis, bit)
        total = blocks[:half].astype(F32) + other.astype(F32)
        bit *= 2
        blocks = total if half == 1 else total.astype(BF16)
    return blocks[0].astype(F32)


def collected(block, axis):
    blocks = block[None]
    bit = lax.axis_size(axis) // 2
    while bit >= 1:
        blocks = jnp.concatenate([blocks, paired(blocks, axis, bit)], axis=0)
        bit //= 2
    return blocks


def local(
    residual,
    small_heads,
    large_heads,
    state_keys,
    state_queries,
    small_gate,
    large_gate,
    small_step,
    large_step,
    small_taps,
    large_taps,
    key_taps,
    query_taps,
    small_decay,
    large_decay,
    small_gain,
    large_gain,
    small_out,
    large_out,
    mixer_gain,
    ffn_in_gain,
    gate_proj,
    up_proj,
    down_proj,
    ffn_out_gain,
):
    length, features = residual.shape
    state_len = state_keys.shape[-1]
    key_rows = state_keys.reshape(length, -1)
    query_rows = state_queries.reshape(length, -1)
    halo_rows = small_taps.shape[0] - 1
    first_row = length - halo_rows
    last = jnp.concatenate(
        [a[first_row:] for a in (small_heads, large_heads, key_rows, query_rows)], axis=1
    )
    halo = earlier(last, "sp", 1)
    halo = jnp.pad(halo, ((HALO - halo_rows, 0), (0, 0)))
    gate_full = lax.all_gather(gate_proj, "sp", axis=0, tiled=True)
    up_full = lax.all_gather(up_proj, "sp", axis=0, tiled=True)
    down_full = lax.all_gather(down_proj, "sp", axis=0, tiled=True)

    heads_a = small_step.shape[1]
    heads_b = large_step.shape[1]
    heads = heads_a + heads_b
    width_a = small_heads.shape[1]
    width_b = large_heads.shape[1]
    width = width_a + width_b
    everything = width + key_rows.shape[1] + query_rows.shape[1]
    sizes = ((heads_a, width_a // heads_a), (heads_b, width_b // heads_b), state_len)
    steps = jnp.pad(
        jnp.concatenate([small_step, large_step], axis=1), ((0, 0), (0, SLOTS - heads))
    )
    steps_across = steps.T
    decay = jnp.pad(jnp.concatenate([small_decay, large_decay]), (0, SLOTS - heads))
    taps = jnp.concatenate(
        [
            small_taps,
            large_taps,
            key_taps.reshape(halo_rows + 1, -1),
            query_taps.reshape(halo_rows + 1, -1),
        ],
        axis=1,
    ).astype(F32)
    gain = jnp.concatenate([small_gain, large_gain]).astype(F32)[None]
    blocks = length // BLOCK

    def rows(columns):
        return pl.BlockSpec((BLOCK, columns), lambda i, *_: (i, 0))

    def whole(*shape):
        return pl.BlockSpec(shape, lambda i, *_: (0,) * len(shape))

    conv, packed = pl.pallas_call(
        functools.partial(conv_kernel, sizes),
        grid=(blocks,),
        in_specs=[
            rows(width_a),
            rows(width_b),
            rows(key_rows.shape[1]),
            rows(query_rows.shape[1]),
            whole(HALO, everything),
            whole(halo_rows + 1, everything),
            rows(SLOTS),
            whole(1, SLOTS),
        ],
        out_specs=[rows(everything), whole(state_len + TAIL, width)],
        out_shape=[
            jax.ShapeDtypeStruct((length, everything), BF16),
            jax.ShapeDtypeStruct((state_len + TAIL, width), BF16),
        ],
        scratch_shapes=[
            pltpu.VMEM((HALO, everything), BF16),
            pltpu.VMEM((state_len, width), F32),
            pltpu.VMEM((1, SLOTS), F32),
        ],
        cost_estimate=pl.CostEstimate(
            flops=10_000_000_000, bytes_accessed=length * everything * 4, transcendentals=0
        ),
        name="convolve",
    )(small_heads, large_heads, key_rows, query_rows, halo, taps, steps, decay[None])

    def opened(array):
        whole_log = array[state_len : state_len + 1].astype(F32)
        whole_log = whole_log + array[state_len + 1 : state_len + 2].astype(F32)
        return array[:state_len].astype(F32), whole_log

    count = lax.axis_size("sp")
    near = 1
    while near * near < count:
        near *= 2
    received = [opened(earlier(packed, "sp", d)) for d in range(1, near + 1)]
    entering, log = received[-1]
    for nearer, nearer_log in received[-2::-1]:
        entering = entering * jnp.exp(nearer_log) + nearer
        log = log + nearer_log
    distance = near
    while distance < count:
        high = lax.reduce_precision(log, 8, 7)
        sent = jnp.concatenate(
            [
                entering.astype(BF16),
                high.astype(BF16),
                (log - high).astype(BF16),
            ],
            axis=0,
        )
        far_state, far_log = opened(earlier(sent, "sp", distance))
        entering = far_state * jnp.exp(log) + entering
        log = log + far_log
        distance *= 2

    share_count = lax.axis_size("tp")
    me = lax.axis_index("tp")
    share = length // share_count
    per_share = share // BLOCK

    def out_place(i, place):
        return (reversed_bits((i // per_share) ^ place[0], share_count), i % per_share, 0)

    partial_value = pl.pallas_call(
        functools.partial(mix_kernel, sizes),
        grid_spec=pltpu.PrefetchScalarGridSpec(
            num_scalar_prefetch=1,
            grid=(blocks,),
            in_specs=[
                rows(everything),
                rows(width_a),
                rows(width_b),
                rows(SLOTS),
                pl.BlockSpec((SLOTS, BLOCK), lambda i, *_: (0, i)),
                whole(1, SLOTS),
                whole(SLOTS, 1),
                whole(1, width),
                whole(width_a, features),
                whole(width_b, features),
                whole(state_len, width),
            ],
            out_specs=pl.BlockSpec((1, BLOCK, features), out_place),
            scratch_shapes=[pltpu.VMEM((state_len, width), F32)],
        ),
        out_shape=jax.ShapeDtypeStruct((share_count, share, features), BF16),
        cost_estimate=pl.CostEstimate(
            flops=10_000_000_000, bytes_accessed=length * features * 4, transcendentals=0
        ),
        name="mix",
    )(
        jnp.reshape(me, (1,)).astype(jnp.int32),
        conv,
        small_gate,
        large_gate,
        steps,
        steps_across,
        decay[None],
        decay[:, None],
        gain,
        small_out,
        large_out,
        entering,
    )
    mix = scattered(partial_value, "tp")
    own = lax.dynamic_slice_in_dim(residual, me * share, share, 0).astype(F32)
    mixed = own + unit_rms(mix) * mixer_gain.astype(F32)
    normed_own = (unit_rms(mixed) * ffn_in_gain.astype(F32)).astype(BF16)
    normed_in = collected(normed_own, "tp").reshape(length, features)
    gate = jnp.dot(normed_in, gate_full, preferred_element_type=F32)
    up_values = jnp.dot(normed_in, up_full, preferred_element_type=F32)
    hidden = (jax.nn.silu(gate) * up_values).astype(BF16)
    parts = lax.dot_general(
        hidden, down_full, (((1,), (1,)), ((), ())), preferred_element_type=F32
    ).astype(BF16)
    ffn = scattered(parts.reshape(share_count, share, features), "tp")
    updated = mixed + 0.5 * unit_rms(ffn) * ffn_out_gain.astype(F32)
    return updated.astype(BF16)


def solution(mesh):
    placed = (
        P("sp", None),
        P("sp", "tp"),
        P("sp", "tp"),
        P("sp", "tp", None),
        P("sp", "tp", None),
        P("sp", "tp"),
        P("sp", "tp"),
        P("sp", "tp"),
        P("sp", "tp"),
        P(None, "tp"),
        P(None, "tp"),
        P(None, "tp", None),
        P(None, "tp", None),
        P("tp"),
        P("tp"),
        P("tp"),
        P("tp"),
        P("tp", None),
        P("tp", None),
        P(),
        P(),
        P("sp", "tp"),
        P("sp", "tp"),
        P("sp", "tp"),
        P(),
    )
    return jax.shard_map(
        local, mesh=mesh, in_specs=placed, out_specs=P(("sp", "tp"), None), check_vma=False
    )
```

```python
import functools

import jax
import jax.numpy as jnp
from jax import lax
from jax.experimental import pallas as pl
from jax.experimental.pallas import tpu as pltpu
from jax.sharding import PartitionSpec as P


BLOCK = 128
HALO = 16
LANES = 128
SLOTS = 8
TAIL = 16


EPS = 1e-06
OUTER, INNER, PARTS = "so", "si", 2
SEQ = (OUTER, INNER)
FAR = -1e30
F32 = jnp.float32
BF16 = jnp.bfloat16


def moved(block, axis, route):
    return lax.ppermute(block, axis, route)


def earlier(block, axis, distance):
    devices = range(lax.axis_size(axis))
    return moved(block, axis, [(i - distance, i) for i in devices if i - distance in devices])


def paired(block, axis, bit):
    return moved(block, axis, [(i, i ^ bit) for i in range(lax.axis_size(axis))])


def silu(x):
    return x / (1.0 + jnp.exp(-x))


def softplus(x):
    return jnp.maximum(x, 0.0) + jnp.log1p(jnp.exp(-jnp.abs(x)))


def exact_dot(a, b):
    return lax.dot_general(
        a, b, (((1,), (0,)), ((), ())), precision=lax.Precision.HIGHEST, preferred_element_type=F32
    )


def lower(n):
    rows = lax.broadcasted_iota(jnp.int32, (n, n), 0)
    return rows >= lax.broadcasted_iota(jnp.int32, (n, n), 1)


def spread(columns, heads, dim):
    rows = columns.shape[0]
    parts = []
    if dim >= LANES:
        for h in heads:
            parts.append(jnp.broadcast_to(columns[:, h : h + 1], (rows, dim)))
    else:
        per = LANES // dim
        lane = lax.broadcasted_iota(jnp.int32, (rows, LANES), 1)
        for first in range(0, len(heads), per):
            part = jnp.broadcast_to(columns[:, heads[first] : heads[first] + 1], (rows, LANES))
            for j in range(1, per):
                h = heads[first + j]
                part = jnp.where(lane >= j * dim, columns[:, h : h + 1], part)
            parts.append(part)
    return jnp.concatenate(parts, axis=1)


def conv_kernel(
    sizes, small, large, keys, queries, halo, taps, steps, decay, conv, packed, before, state, total
):
    (heads_a, dim_a), (heads_b, dim_b), state_len = sizes
    step = pl.program_id(0)

    @pl.when(step == 0)
    def _():
        before[...] = halo[...]
        state[...] = jnp.zeros_like(state)
        total[...] = jnp.zeros_like(total)

    column = 0
    for ref in (small, large, keys, queries):
        width = ref.shape[1]
        for start in range(0, width, LANES):
            here = pl.ds(column, LANES)
            now = ref[:, pl.ds(start, LANES)]
            extended = jnp.concatenate([before[:, here], now], axis=0).astype(F32)
            kernel_len = taps.shape[0]
            summed = None
            for k in range(kernel_len):
                first = HALO - kernel_len + 1 + k
                term = taps[k : k + 1, here] * extended[first : first + BLOCK]
                summed = term if summed is None else summed + term
            done = silu(summed).astype(BF16)
            conv[:, here] = done
            before[:, here] = now[BLOCK - HALO :]
            column += LANES
    dt = softplus(steps[...])
    cum = exact_dot(lower(BLOCK).astype(F32), -dt * jnp.exp(decay[...]))
    tail = cum[BLOCK - 1 : BLOCK]
    scale = dt * jnp.exp(tail - cum)
    head_list_a = list(range(heads_a))
    head_list_b = list(range(heads_a, heads_a + heads_b))
    kept = jnp.exp(tail)
    offset = 0
    width_a = heads_a * dim_a
    width_b = heads_b * dim_b
    for heads, dim, width, key_at in (
        (head_list_a, dim_a, width_a, width_a + width_b),
        (head_list_b, dim_b, width_b, width_a + width_b + state_len),
    ):
        x = conv[:, offset : offset + width].astype(F32)
        u = (x * spread(scale, heads, dim)).astype(BF16)
        k = conv[:, key_at : key_at + state_len]
        fresh = lax.dot_general(k, u, (((0,), (0,)), ((), ())), preferred_element_type=F32)
        old = state[:, offset : offset + width]
        state[:, offset : offset + width] = old * spread(kept, heads, dim) + fresh
        offset += width
    total[...] = total[...] + tail

    @pl.when(step == pl.num_programs(0) - 1)
    def _():
        packed[:state_len] = state[...].astype(BF16)
        whole = jnp.concatenate(
            [spread(total[...], head_list_a, dim_a), spread(total[...], head_list_b, dim_b)], axis=1
        )
        high = whole.astype(BF16)
        low = (whole - high.astype(F32)).astype(BF16)
        row = lax.broadcasted_iota(jnp.int32, (TAIL, whole.shape[1]), 0)
        both = jnp.where(row == 0, high.astype(F32), jnp.where(row == 1, low.astype(F32), 0.0))
        packed[state_len:] = both.astype(BF16)


def mix_kernel(
    sizes,
    place,
    conv,
    small_gate,
    large_gate,
    steps,
    steps_across,
    decay,
    decay_across,
    gain,
    small_out,
    large_out,
    entering,
    partial_out,
    state,
):
    (heads_a, dim_a), (heads_b, dim_b), state_len = sizes
    step = pl.program_id(0)

    @pl.when(step == 0)
    def _():
        state[...] = entering[...]

    causal = lower(BLOCK)
    ones = causal.astype(F32)
    dt = softplus(steps[...])
    cum = exact_dot(ones, -dt * jnp.exp(decay[...]))
    dt_across = softplus(steps_across[...])
    upper = (
        lax.broadcasted_iota(jnp.int32, (BLOCK, BLOCK), 0)
        <= lax.broadcasted_iota(jnp.int32, (BLOCK, BLOCK), 1)
    ).astype(F32)
    cum_across = exact_dot(-dt_across * jnp.exp(decay_across[...]), upper)
    tail = cum[BLOCK - 1 : BLOCK]
    scale = dt * jnp.exp(tail - cum)
    grown = jnp.exp(cum)
    kept = jnp.exp(tail)
    width_a = heads_a * dim_a
    width_b = heads_b * dim_b
    offset = 0
    result = None
    lane = lax.broadcasted_iota(jnp.int32, (BLOCK, LANES), 1)
    for which, (heads, dim, width, gate, out) in enumerate(
        (
            (list(range(heads_a)), dim_a, width_a, small_gate, small_out),
            (list(range(heads_a, heads_a + heads_b)), dim_b, width_b, large_gate, large_out),
        )
    ):
        key_at = width_a + width_b + which * state_len
        query_at = key_at + 2 * state_len
        x = conv[:, offset : offset + width]
        k = conv[:, key_at : key_at + state_len]
        q = conv[:, query_at : query_at + state_len]
        scores = lax.dot_general(q, k, (((1,), (1,)), ((), ())), preferred_element_type=F32)
        old = state[:, offset : offset + width]
        carried = jnp.dot(q, old.astype(BF16), preferred_element_type=F32)
        carried = carried * spread(grown, heads, dim)
        u = (x.astype(F32) * spread(scale, heads, dim)).astype(BF16)
        fresh = lax.dot_general(k, u, (((0,), (0,)), ((), ())), preferred_element_type=F32)
        state[:, offset : offset + width] = old * spread(kept, heads, dim) + fresh
        inside = []
        span = max(dim, LANES)
        per = span // dim
        for first in range(0, len(heads), per):
            x_part = x[:, first * dim : first * dim + span]
            part = None
            for j in range(per):
                h = heads[first + j]
                gap = cum[:, h : h + 1] - cum_across[h : h + 1]
                decays = jnp.exp(jnp.where(causal, gap, FAR))
                w = (scores * decays * dt_across[h : h + 1]).astype(BF16)
                got = jnp.dot(w, x_part, preferred_element_type=F32)
                part = got if part is None else jnp.where(lane >= j * dim, got, part)
            inside.append(part)
        mixed = jnp.concatenate(inside, axis=1) + carried
        gated = mixed * silu(gate[...].astype(F32))
        squares = gated * gated
        normed = []
        for first in range(0, len(heads), per):
            at = first * dim
            part = squares[:, at : at + span]
            means = None
            for j in range(per):
                if per == 1:
                    means = jnp.sum(part, axis=1, keepdims=True)
                else:
                    ours = (lane >= j * dim) & (lane < (j + 1) * dim)
                    one = jnp.sum(jnp.where(ours, part, 0.0), axis=1, keepdims=True)
                    means = one if means is None else jnp.where(lane >= j * dim, one, means)
            normed.append(gated[:, at : at + span] * lax.rsqrt(means * (1.0 / dim) + EPS))
        normed = jnp.concatenate(normed, axis=1) * gain[:, offset : offset + width]
        product = jnp.dot(normed.astype(BF16), out[...], preferred_element_type=F32)
        result = product if result is None else result + product
        offset += width
    partial_out[...] = result.astype(BF16)[None]


def unit_rms(values):
    return values * lax.rsqrt(jnp.mean(values * values, axis=-1, keepdims=True) + EPS)


def reversed_bits(value, count):
    out = 0
    bit = 1
    while bit < count:
        out = out * 2 + (value // bit) % 2
        bit *= 2
    return out


def scattered(blocks, axis):
    bit = 1
    while blocks.shape[0] > 1:
        half = blocks.shape[0] // 2
        other = paired(blocks[half:], axis, bit)
        total = blocks[:half].astype(F32) + other.astype(F32)
        bit *= 2
        blocks = total if half == 1 else total.astype(BF16)
    return blocks[0].astype(F32)


def collected(block, axis):
    blocks = block[None]
    bit = lax.axis_size(axis) // 2
    while bit >= 1:
        other = paired(blocks, axis, bit)
        blocks = jnp.concatenate([blocks, other], axis=0)
        bit //= 2
    return blocks


def layer(
    residual,
    small_heads,
    large_heads,
    state_keys,
    state_queries,
    small_gate,
    large_gate,
    small_step,
    large_step,
    small_taps,
    large_taps,
    key_taps,
    query_taps,
    small_decay,
    large_decay,
    small_gain,
    large_gain,
    small_out,
    large_out,
    mixer_gain,
    ffn_in_gain,
    gate_proj,
    up_proj,
    down_proj,
    ffn_out_gain,
):
    length, features = residual.shape
    state_len = state_keys.shape[-1]
    key_rows = state_keys.reshape(length, -1)
    query_rows = state_queries.reshape(length, -1)
    halo_rows = small_taps.shape[0] - 1
    first_row = length - halo_rows
    last = jnp.concatenate(
        [a[first_row:] for a in (small_heads, large_heads, key_rows, query_rows)], axis=1
    )
    halo = earlier(last, SEQ, 1)
    halo = jnp.pad(halo, ((HALO - halo_rows, 0), (0, 0)))
    side = lax.axis_index(INNER)
    down_other = paired(down_proj, INNER, 1)
    down_pair = jnp.where(
        side == 0, jnp.stack([down_proj, down_other]), jnp.stack([down_other, down_proj])
    )
    gate_mine = lax.all_gather(gate_proj, OUTER, axis=0, tiled=True)
    up_mine = lax.all_gather(up_proj, OUTER, axis=0, tiled=True)
    own_rows = down_proj.shape[0]
    piece = own_rows // PARTS
    down_parts = []
    for p in range(PARTS):
        sent = down_pair[:, p * piece : (p + 1) * piece].reshape(2 * piece, -1)
        down_parts.append(lax.all_gather(sent, OUTER, axis=0, tiled=True))
    gate_theirs = paired(gate_mine, INNER, 1)
    up_theirs = paired(up_mine, INNER, 1)

    heads_a = small_step.shape[1]
    heads_b = large_step.shape[1]
    heads = heads_a + heads_b
    width_a = small_heads.shape[1]
    width_b = large_heads.shape[1]
    width = width_a + width_b
    everything = width + key_rows.shape[1] + query_rows.shape[1]
    sizes = ((heads_a, width_a // heads_a), (heads_b, width_b // heads_b), state_len)
    steps = jnp.pad(
        jnp.concatenate([small_step, large_step], axis=1), ((0, 0), (0, SLOTS - heads))
    )
    steps_across = steps.T
    decay = jnp.pad(jnp.concatenate([small_decay, large_decay]), (0, SLOTS - heads))
    taps = jnp.concatenate(
        [
            small_taps,
            large_taps,
            key_taps.reshape(halo_rows + 1, -1),
            query_taps.reshape(halo_rows + 1, -1),
        ],
        axis=1,
    ).astype(F32)
    gain = jnp.concatenate([small_gain, large_gain]).astype(F32)[None]
    blocks = length // BLOCK

    def rows(columns):
        return pl.BlockSpec((BLOCK, columns), lambda i, *_: (i, 0))

    def whole(*shape):
        return pl.BlockSpec(shape, lambda i, *_: (0,) * len(shape))

    conv, packed = pl.pallas_call(
        functools.partial(conv_kernel, sizes),
        grid=(blocks,),
        in_specs=[
            rows(width_a),
            rows(width_b),
            rows(key_rows.shape[1]),
            rows(query_rows.shape[1]),
            whole(HALO, everything),
            whole(halo_rows + 1, everything),
            rows(SLOTS),
            whole(1, SLOTS),
        ],
        out_specs=[rows(everything), whole(state_len + TAIL, width)],
        out_shape=[
            jax.ShapeDtypeStruct((length, everything), BF16),
            jax.ShapeDtypeStruct((state_len + TAIL, width), BF16),
        ],
        scratch_shapes=[
            pltpu.VMEM((HALO, everything), BF16),
            pltpu.VMEM((state_len, width), F32),
            pltpu.VMEM((1, SLOTS), F32),
        ],
        cost_estimate=pl.CostEstimate(
            flops=10_000_000_000, bytes_accessed=length * everything * 4, transcendentals=0
        ),
        name="convolve",
    )(small_heads, large_heads, key_rows, query_rows, halo, taps, steps, decay[None])

    def opened(array):
        whole_log = array[state_len : state_len + 1].astype(F32)
        whole_log = whole_log + array[state_len + 1 : state_len + 2].astype(F32)
        return array[:state_len].astype(F32), whole_log

    count = lax.axis_size(SEQ)
    near = 1
    while near * near < count:
        near *= 2
    received = [opened(earlier(packed, SEQ, d)) for d in range(1, near + 1)]
    entering, log = received[-1]
    for nearer, nearer_log in received[-2::-1]:
        entering = entering * jnp.exp(nearer_log) + nearer
        log = log + nearer_log
    distance = near
    while distance < count:
        high = lax.reduce_precision(log, 8, 7)
        sent = jnp.concatenate(
            [
                entering.astype(BF16),
                high.astype(BF16),
                (log - high).astype(BF16),
            ],
            axis=0,
        )
        far_state, far_log = opened(earlier(sent, SEQ, distance))
        entering = far_state * jnp.exp(log) + entering
        log = log + far_log
        distance *= 2

    share_count = lax.axis_size("tp")
    me = lax.axis_index("tp")
    share = length // share_count
    per_share = share // BLOCK

    def out_place(i, place):
        return (reversed_bits((i // per_share) ^ place[0], share_count), i % per_share, 0)

    partial_value = pl.pallas_call(
        functools.partial(mix_kernel, sizes),
        grid_spec=pltpu.PrefetchScalarGridSpec(
            num_scalar_prefetch=1,
            grid=(blocks,),
            in_specs=[
                rows(everything),
                rows(width_a),
                rows(width_b),
                rows(SLOTS),
                pl.BlockSpec((SLOTS, BLOCK), lambda i, *_: (0, i)),
                whole(1, SLOTS),
                whole(SLOTS, 1),
                whole(1, width),
                whole(width_a, features),
                whole(width_b, features),
                whole(state_len, width),
            ],
            out_specs=pl.BlockSpec((1, BLOCK, features), out_place),
            scratch_shapes=[pltpu.VMEM((state_len, width), F32)],
        ),
        out_shape=jax.ShapeDtypeStruct((share_count, share, features), BF16),
        cost_estimate=pl.CostEstimate(
            flops=10_000_000_000, bytes_accessed=length * features * 4, transcendentals=0
        ),
        name="mix",
    )(
        jnp.reshape(me, (1,)).astype(jnp.int32),
        conv,
        small_gate,
        large_gate,
        steps,
        steps_across,
        decay[None],
        decay[:, None],
        gain,
        small_out,
        large_out,
        entering,
    )
    mix = scattered(partial_value, "tp")
    own = lax.dynamic_slice_in_dim(residual, me * share, share, 0).astype(F32)
    mixed = own + unit_rms(mix) * mixer_gain.astype(F32)
    normed_own = unit_rms(mixed) * ffn_in_gain.astype(F32)
    cut = normed_own.astype(BF16).reshape(share, -1, 2, own_rows)
    first, second = cut[:, :, 0], cut[:, :, 1]
    normed_own = jnp.stack(
        [jnp.where(side == 0, first, second), jnp.where(side == 0, second, first)], axis=1
    ).reshape(share, features)
    normed_in = collected(normed_own, "tp").reshape(length, features)
    half = features // 2
    mine, theirs = normed_in[:, :half], normed_in[:, half:]
    gate = jnp.dot(mine, gate_mine, preferred_element_type=F32)
    up_values = jnp.dot(mine, up_mine, preferred_element_type=F32)
    gate = gate + jnp.dot(theirs, gate_theirs, preferred_element_type=F32)
    up_values = up_values + jnp.dot(theirs, up_theirs, preferred_element_type=F32)
    hidden = (jax.nn.silu(gate) * up_values).astype(BF16)
    sums = []
    for down in down_parts:
        parts = lax.dot_general(
            hidden, down, (((1,), (1,)), ((), ())), preferred_element_type=F32
        ).astype(BF16)
        sums.append(scattered(parts.reshape(share_count, share, -1), "tp"))
    squares = sum(jnp.sum(part * part, axis=-1, keepdims=True) for part in sums)
    ffn_scale = 0.5 * lax.rsqrt(squares * (1.0 / features) + EPS)
    ffn = jnp.stack([part.reshape(share, -1, piece) for part in sums], axis=2)
    ffn = ffn.reshape(share, features)
    updated = mixed + ffn * ffn_scale * ffn_out_gain.astype(F32)
    return updated.astype(BF16)


def solution(mesh):
    placed = (
        P(SEQ, None),
        P(SEQ, "tp"),
        P(SEQ, "tp"),
        P(SEQ, "tp", None),
        P(SEQ, "tp", None),
        P(SEQ, "tp"),
        P(SEQ, "tp"),
        P(SEQ, "tp"),
        P(SEQ, "tp"),
        P(None, "tp"),
        P(None, "tp"),
        P(None, "tp", None),
        P(None, "tp", None),
        P("tp"),
        P("tp"),
        P("tp"),
        P("tp"),
        P("tp", None),
        P("tp", None),
        P(),
        P(),
        P(SEQ, "tp"),
        P(SEQ, "tp"),
        P(SEQ, "tp"),
        P(),
    )
    inner = 2
    outer = mesh.shape["sp"] // inner
    cut = jax.sharding.Mesh(
        mesh.devices.reshape(outer, inner, mesh.shape["tp"]), (OUTER, INNER, "tp")
    )
    return jax.shard_map(
        layer, mesh=cut, in_specs=placed, out_specs=P((*SEQ, "tp"), None), check_vma=False
    )
```

```python
import functools

import jax
import jax.numpy as jnp
from jax import lax
from jax.experimental import pallas as pl
from jax.experimental.pallas import tpu as pltpu
from jax.sharding import PartitionSpec as P


BLOCK = 128
HALO = 16
LANES = 128
SLOTS = 8
TAIL = 16


EPS = 1e-06
OUTER, INNER, PARTS = "so", "si", 2
SEQ = (OUTER, INNER)
FAR = -1e30
F32 = jnp.float32
BF16 = jnp.bfloat16


def moved(block, axis, route):
    return lax.ppermute(block, axis, route)


def earlier(block, axis, distance):
    devices = range(lax.axis_size(axis))
    return moved(block, axis, [(i - distance, i) for i in devices if i - distance in devices])


def paired(block, axis, bit):
    return moved(block, axis, [(i, i ^ bit) for i in range(lax.axis_size(axis))])


def silu(x):
    return x / (1.0 + jnp.exp(-x))


def softplus(x):
    return jnp.maximum(x, 0.0) + jnp.log1p(jnp.exp(-jnp.abs(x)))


def exact_dot(a, b):
    return lax.dot_general(
        a, b, (((1,), (0,)), ((), ())), precision=lax.Precision.HIGHEST, preferred_element_type=F32
    )


def lower(n):
    rows = lax.broadcasted_iota(jnp.int32, (n, n), 0)
    return rows >= lax.broadcasted_iota(jnp.int32, (n, n), 1)


def spread(columns, heads, dim):
    rows = columns.shape[0]
    parts = []
    if dim >= LANES:
        for h in heads:
            parts.append(jnp.broadcast_to(columns[:, h : h + 1], (rows, dim)))
    else:
        per = LANES // dim
        lane = lax.broadcasted_iota(jnp.int32, (rows, LANES), 1)
        for first in range(0, len(heads), per):
            part = jnp.broadcast_to(columns[:, heads[first] : heads[first] + 1], (rows, LANES))
            for j in range(1, per):
                h = heads[first + j]
                part = jnp.where(lane >= j * dim, columns[:, h : h + 1], part)
            parts.append(part)
    return jnp.concatenate(parts, axis=1)


def conv_kernel(
    sizes, small, large, keys, queries, halo, taps, steps, decay, conv, packed, before, state, total
):
    (heads_a, dim_a), (heads_b, dim_b), state_len = sizes
    step = pl.program_id(0)

    @pl.when(step == 0)
    def _():
        before[...] = halo[...]
        state[...] = jnp.zeros_like(state)
        total[...] = jnp.zeros_like(total)

    column = 0
    for ref in (small, large, keys, queries):
        width = ref.shape[1]
        for start in range(0, width, LANES):
            here = pl.ds(column, LANES)
            now = ref[:, pl.ds(start, LANES)]
            extended = jnp.concatenate([before[:, here], now], axis=0).astype(F32)
            kernel_len = taps.shape[0]
            summed = None
            for k in range(kernel_len):
                first = HALO - kernel_len + 1 + k
                term = taps[k : k + 1, here] * extended[first : first + BLOCK]
                summed = term if summed is None else summed + term
            done = silu(summed).astype(BF16)
            conv[:, here] = done
            before[:, here] = now[BLOCK - HALO :]
            column += LANES
    dt = softplus(steps[...])
    cum = exact_dot(lower(BLOCK).astype(F32), -dt * jnp.exp(decay[...]))
    tail = cum[BLOCK - 1 : BLOCK]
    scale = dt * jnp.exp(tail - cum)
    head_list_a = list(range(heads_a))
    head_list_b = list(range(heads_a, heads_a + heads_b))
    kept = jnp.exp(tail)
    offset = 0
    width_a = heads_a * dim_a
    width_b = heads_b * dim_b
    for heads, dim, width, key_at in (
        (head_list_a, dim_a, width_a, width_a + width_b),
        (head_list_b, dim_b, width_b, width_a + width_b + state_len),
    ):
        x = conv[:, offset : offset + width].astype(F32)
        u = (x * spread(scale, heads, dim)).astype(BF16)
        k = conv[:, key_at : key_at + state_len]
        fresh = lax.dot_general(k, u, (((0,), (0,)), ((), ())), preferred_element_type=F32)
        old = state[:, offset : offset + width]
        state[:, offset : offset + width] = old * spread(kept, heads, dim) + fresh
        offset += width
    total[...] = total[...] + tail

    @pl.when(step == pl.num_programs(0) - 1)
    def _():
        packed[:state_len] = state[...].astype(BF16)
        whole = jnp.concatenate(
            [spread(total[...], head_list_a, dim_a), spread(total[...], head_list_b, dim_b)], axis=1
        )
        high = whole.astype(BF16)
        low = (whole - high.astype(F32)).astype(BF16)
        row = lax.broadcasted_iota(jnp.int32, (TAIL, whole.shape[1]), 0)
        both = jnp.where(row == 0, high.astype(F32), jnp.where(row == 1, low.astype(F32), 0.0))
        packed[state_len:] = both.astype(BF16)


def mix_kernel(
    sizes,
    place,
    conv,
    small_gate,
    large_gate,
    steps,
    steps_across,
    decay,
    decay_across,
    gain,
    small_out,
    large_out,
    entering,
    partial_out,
    state,
):
    (heads_a, dim_a), (heads_b, dim_b), state_len = sizes
    step = pl.program_id(0)

    @pl.when(step == 0)
    def _():
        state[...] = entering[...]

    causal = lower(BLOCK)
    ones = causal.astype(F32)
    dt = softplus(steps[...])
    cum = exact_dot(ones, -dt * jnp.exp(decay[...]))
    dt_across = softplus(steps_across[...])
    upper = (
        lax.broadcasted_iota(jnp.int32, (BLOCK, BLOCK), 0)
        <= lax.broadcasted_iota(jnp.int32, (BLOCK, BLOCK), 1)
    ).astype(F32)
    cum_across = exact_dot(-dt_across * jnp.exp(decay_across[...]), upper)
    tail = cum[BLOCK - 1 : BLOCK]
    scale = dt * jnp.exp(tail - cum)
    grown = jnp.exp(cum)
    kept = jnp.exp(tail)
    width_a = heads_a * dim_a
    width_b = heads_b * dim_b
    offset = 0
    result = None
    lane = lax.broadcasted_iota(jnp.int32, (BLOCK, LANES), 1)
    for which, (heads, dim, width, gate, out) in enumerate(
        (
            (list(range(heads_a)), dim_a, width_a, small_gate, small_out),
            (list(range(heads_a, heads_a + heads_b)), dim_b, width_b, large_gate, large_out),
        )
    ):
        key_at = width_a + width_b + which * state_len
        query_at = key_at + 2 * state_len
        x = conv[:, offset : offset + width]
        k = conv[:, key_at : key_at + state_len]
        q = conv[:, query_at : query_at + state_len]
        scores = lax.dot_general(q, k, (((1,), (1,)), ((), ())), preferred_element_type=F32)
        old = state[:, offset : offset + width]
        carried = jnp.dot(q, old.astype(BF16), preferred_element_type=F32)
        carried = carried * spread(grown, heads, dim)
        u = (x.astype(F32) * spread(scale, heads, dim)).astype(BF16)
        fresh = lax.dot_general(k, u, (((0,), (0,)), ((), ())), preferred_element_type=F32)
        state[:, offset : offset + width] = old * spread(kept, heads, dim) + fresh
        inside = []
        span = max(dim, LANES)
        per = span // dim
        for first in range(0, len(heads), per):
            x_part = x[:, first * dim : first * dim + span]
            part = None
            for j in range(per):
                h = heads[first + j]
                gap = cum[:, h : h + 1] - cum_across[h : h + 1]
                decays = jnp.exp(jnp.where(causal, gap, FAR))
                w = (scores * decays * dt_across[h : h + 1]).astype(BF16)
                got = jnp.dot(w, x_part, preferred_element_type=F32)
                part = got if part is None else jnp.where(lane >= j * dim, got, part)
            inside.append(part)
        mixed = jnp.concatenate(inside, axis=1) + carried
        gated = mixed * silu(gate[...].astype(F32))
        squares = gated * gated
        normed = []
        for first in range(0, len(heads), per):
            at = first * dim
            part = squares[:, at : at + span]
            means = None
            for j in range(per):
                if per == 1:
                    means = jnp.sum(part, axis=1, keepdims=True)
                else:
                    ours = (lane >= j * dim) & (lane < (j + 1) * dim)
                    one = jnp.sum(jnp.where(ours, part, 0.0), axis=1, keepdims=True)
                    means = one if means is None else jnp.where(lane >= j * dim, one, means)
            normed.append(gated[:, at : at + span] * lax.rsqrt(means * (1.0 / dim) + EPS))
        normed = jnp.concatenate(normed, axis=1) * gain[:, offset : offset + width]
        product = jnp.dot(normed.astype(BF16), out[...], preferred_element_type=F32)
        result = product if result is None else result + product
        offset += width
    partial_out[...] = result.astype(BF16)[None]


def unit_rms(values):
    return values * lax.rsqrt(jnp.mean(values * values, axis=-1, keepdims=True) + EPS)


def norm_kernel(chunk, side, one, other, own, mixer_gain, ffn_gain, mixed_out, normed_out):
    mix = one[...].astype(F32) + other[...].astype(F32)
    mixed = own[...].astype(F32) + unit_rms(mix) * mixer_gain[...].astype(F32)
    mixed_out[...] = mixed
    normed = (unit_rms(mixed) * ffn_gain[...].astype(F32)).astype(BF16)
    half = normed.shape[1] // 2
    for j in range(half // chunk):
        first = normed[:, 2 * j * chunk : (2 * j + 1) * chunk]
        second = normed[:, (2 * j + 1) * chunk : (2 * j + 2) * chunk]
        at = j * chunk

        @pl.when(side[0] == 0)
        def _():
            normed_out[:, at : at + chunk] = first
            normed_out[:, half + at : half + at + chunk] = second

        @pl.when(side[0] != 0)
        def _():
            normed_out[:, at : at + chunk] = second
            normed_out[:, half + at : half + at + chunk] = first


def last_kernel(piece, *refs):
    *terms, mixed, gain, out = refs
    sums = []
    for p in range(PARTS):
        sums.append(terms[2 * p][...].astype(F32) + terms[2 * p + 1][...].astype(F32))
    features = mixed.shape[1]
    squares = sum(jnp.sum(part * part, axis=-1, keepdims=True) for part in sums)
    scale = 0.5 * lax.rsqrt(squares * (1.0 / features) + EPS)
    for j in range(features // piece):
        at = j * piece
        here = j // PARTS * piece
        value = sums[j % PARTS][:, here : here + piece] * scale
        value = value * gain[:, at : at + piece].astype(F32)
        out[:, at : at + piece] = (mixed[:, at : at + piece] + value).astype(BF16)


def reversed_bits(value, count):
    out = 0
    bit = 1
    while bit < count:
        out = out * 2 + (value // bit) % 2
        bit *= 2
    return out


def scattered(blocks, axis):
    bit = 1
    while True:
        half = blocks.shape[0] // 2
        other = paired(blocks[half:], axis, bit)
        if half == 1:
            return blocks[0], other[0]
        blocks = (blocks[:half].astype(F32) + other.astype(F32)).astype(BF16)
        bit *= 2


def collected(block, axis):
    blocks = block[None]
    bit = lax.axis_size(axis) // 2
    while bit >= 1:
        other = paired(blocks, axis, bit)
        blocks = jnp.concatenate([blocks, other], axis=0)
        bit //= 2
    return blocks


def layer(
    residual,
    small_heads,
    large_heads,
    state_keys,
    state_queries,
    small_gate,
    large_gate,
    small_step,
    large_step,
    small_taps,
    large_taps,
    key_taps,
    query_taps,
    small_decay,
    large_decay,
    small_gain,
    large_gain,
    small_out,
    large_out,
    mixer_gain,
    ffn_in_gain,
    gate_proj,
    up_proj,
    down_proj,
    ffn_out_gain,
):
    length, features = residual.shape
    state_len = state_keys.shape[-1]
    key_rows = state_keys.reshape(length, -1)
    query_rows = state_queries.reshape(length, -1)
    halo_rows = small_taps.shape[0] - 1
    first_row = length - halo_rows
    last = jnp.concatenate(
        [a[first_row:] for a in (small_heads, large_heads, key_rows, query_rows)], axis=1
    )
    halo = earlier(last, SEQ, 1)
    halo = jnp.pad(halo, ((HALO - halo_rows, 0), (0, 0)))
    side = lax.axis_index(INNER)
    down_other = paired(down_proj, INNER, 1)
    down_pair = jnp.where(
        side == 0, jnp.stack([down_proj, down_other]), jnp.stack([down_other, down_proj])
    )
    gate_mine = lax.all_gather(gate_proj, OUTER, axis=0, tiled=True)
    up_mine = lax.all_gather(up_proj, OUTER, axis=0, tiled=True)
    own_rows = down_proj.shape[0]
    piece = own_rows // PARTS
    down_parts = []
    for p in range(PARTS):
        sent = down_pair[:, p * piece : (p + 1) * piece].reshape(2 * piece, -1)
        down_parts.append(lax.all_gather(sent, OUTER, axis=0, tiled=True))
    gate_theirs = paired(gate_mine, INNER, 1)
    up_theirs = paired(up_mine, INNER, 1)

    heads_a = small_step.shape[1]
    heads_b = large_step.shape[1]
    heads = heads_a + heads_b
    width_a = small_heads.shape[1]
    width_b = large_heads.shape[1]
    width = width_a + width_b
    everything = width + key_rows.shape[1] + query_rows.shape[1]
    sizes = ((heads_a, width_a // heads_a), (heads_b, width_b // heads_b), state_len)
    steps = jnp.pad(
        jnp.concatenate([small_step, large_step], axis=1), ((0, 0), (0, SLOTS - heads))
    )
    steps_across = steps.T
    decay = jnp.pad(jnp.concatenate([small_decay, large_decay]), (0, SLOTS - heads))
    taps = jnp.concatenate(
        [
            small_taps,
            large_taps,
            key_taps.reshape(halo_rows + 1, -1),
            query_taps.reshape(halo_rows + 1, -1),
        ],
        axis=1,
    ).astype(F32)
    gain = jnp.concatenate([small_gain, large_gain]).astype(F32)[None]
    blocks = length // BLOCK

    def rows(columns):
        return pl.BlockSpec((BLOCK, columns), lambda i, *_: (i, 0))

    def whole(*shape):
        return pl.BlockSpec(shape, lambda i, *_: (0,) * len(shape))

    conv, packed = pl.pallas_call(
        functools.partial(conv_kernel, sizes),
        grid=(blocks,),
        in_specs=[
            rows(width_a),
            rows(width_b),
            rows(key_rows.shape[1]),
            rows(query_rows.shape[1]),
            whole(HALO, everything),
            whole(halo_rows + 1, everything),
            rows(SLOTS),
            whole(1, SLOTS),
        ],
        out_specs=[rows(everything), whole(state_len + TAIL, width)],
        out_shape=[
            jax.ShapeDtypeStruct((length, everything), BF16),
            jax.ShapeDtypeStruct((state_len + TAIL, width), BF16),
        ],
        scratch_shapes=[
            pltpu.VMEM((HALO, everything), BF16),
            pltpu.VMEM((state_len, width), F32),
            pltpu.VMEM((1, SLOTS), F32),
        ],
        cost_estimate=pl.CostEstimate(
            flops=10_000_000_000, bytes_accessed=length * everything * 4, transcendentals=0
        ),
        name="convolve",
    )(small_heads, large_heads, key_rows, query_rows, halo, taps, steps, decay[None])

    def opened(array):
        whole_log = array[state_len : state_len + 1].astype(F32)
        whole_log = whole_log + array[state_len + 1 : state_len + 2].astype(F32)
        return array[:state_len].astype(F32), whole_log

    count = lax.axis_size(SEQ)
    near = 1
    while near * near < count:
        near *= 2
    received = [opened(earlier(packed, SEQ, d)) for d in range(1, near + 1)]
    entering, log = received[-1]
    for nearer, nearer_log in received[-2::-1]:
        entering = entering * jnp.exp(nearer_log) + nearer
        log = log + nearer_log
    distance = near
    while distance < count:
        high = lax.reduce_precision(log, 8, 7)
        sent = jnp.concatenate(
            [
                entering.astype(BF16),
                high.astype(BF16),
                (log - high).astype(BF16),
            ],
            axis=0,
        )
        far_state, far_log = opened(earlier(sent, SEQ, distance))
        entering = far_state * jnp.exp(log) + entering
        log = log + far_log
        distance *= 2

    share_count = lax.axis_size("tp")
    me = lax.axis_index("tp")
    share = length // share_count
    per_share = share // BLOCK

    def out_place(i, place):
        return (reversed_bits((i // per_share) ^ place[0], share_count), i % per_share, 0)

    partial_value = pl.pallas_call(
        functools.partial(mix_kernel, sizes),
        grid_spec=pltpu.PrefetchScalarGridSpec(
            num_scalar_prefetch=1,
            grid=(blocks,),
            in_specs=[
                rows(everything),
                rows(width_a),
                rows(width_b),
                rows(SLOTS),
                pl.BlockSpec((SLOTS, BLOCK), lambda i, *_: (0, i)),
                whole(1, SLOTS),
                whole(SLOTS, 1),
                whole(1, width),
                whole(width_a, features),
                whole(width_b, features),
                whole(state_len, width),
            ],
            out_specs=pl.BlockSpec((1, BLOCK, features), out_place),
            scratch_shapes=[pltpu.VMEM((state_len, width), F32)],
        ),
        out_shape=jax.ShapeDtypeStruct((share_count, share, features), BF16),
        cost_estimate=pl.CostEstimate(
            flops=10_000_000_000, bytes_accessed=length * features * 4, transcendentals=0
        ),
        name="mix",
    )(
        jnp.reshape(me, (1,)).astype(jnp.int32),
        conv,
        small_gate,
        large_gate,
        steps,
        steps_across,
        decay[None],
        decay[:, None],
        gain,
        small_out,
        large_out,
        entering,
    )
    mix_one, mix_other = scattered(partial_value, "tp")
    own = lax.dynamic_slice_in_dim(residual, me * share, share, 0)
    tile = BLOCK // 2

    def strips(columns):
        return pl.BlockSpec((tile, columns), lambda i, *_: (i, 0))

    mixed, normed_own = pl.pallas_call(
        functools.partial(norm_kernel, own_rows),
        grid_spec=pltpu.PrefetchScalarGridSpec(
            num_scalar_prefetch=1,
            grid=(share // tile,),
            in_specs=[strips(features)] * 3 + [whole(1, features)] * 2,
            out_specs=[strips(features)] * 2,
        ),
        out_shape=[
            jax.ShapeDtypeStruct((share, features), F32),
            jax.ShapeDtypeStruct((share, features), BF16),
        ],
        cost_estimate=pl.CostEstimate(
            flops=1_000_000_000, bytes_accessed=share * features * 12, transcendentals=0
        ),
        name="norms",
    )(
        jnp.reshape(side, (1,)).astype(jnp.int32),
        mix_one,
        mix_other,
        own,
        mixer_gain[None],
        ffn_in_gain[None],
    )
    normed_in = collected(normed_own, "tp").reshape(length, features)
    half = features // 2
    mine, theirs = normed_in[:, :half], normed_in[:, half:]
    gate = jnp.dot(mine, gate_mine, preferred_element_type=F32)
    up_values = jnp.dot(mine, up_mine, preferred_element_type=F32)
    gate = gate + jnp.dot(theirs, gate_theirs, preferred_element_type=F32)
    up_values = up_values + jnp.dot(theirs, up_theirs, preferred_element_type=F32)
    hidden = (jax.nn.silu(gate) * up_values).astype(BF16)
    sums = []
    for down in down_parts:
        parts = lax.dot_general(
            hidden, down, (((1,), (1,)), ((), ())), preferred_element_type=F32
        ).astype(BF16)
        sums.extend(scattered(parts.reshape(share_count, share, -1), "tp"))
    return pl.pallas_call(
        functools.partial(last_kernel, piece),
        grid=(share // tile,),
        in_specs=[strips(features // PARTS)] * (2 * PARTS) + [strips(features), whole(1, features)],
        out_specs=strips(features),
        out_shape=jax.ShapeDtypeStruct((share, features), BF16),
        cost_estimate=pl.CostEstimate(
            flops=1_000_000_000, bytes_accessed=share * features * 10, transcendentals=0
        ),
        name="last",
    )(*sums, mixed, ffn_out_gain[None])


def solution(mesh):
    placed = (
        P(SEQ, None),
        P(SEQ, "tp"),
        P(SEQ, "tp"),
        P(SEQ, "tp", None),
        P(SEQ, "tp", None),
        P(SEQ, "tp"),
        P(SEQ, "tp"),
        P(SEQ, "tp"),
        P(SEQ, "tp"),
        P(None, "tp"),
        P(None, "tp"),
        P(None, "tp", None),
        P(None, "tp", None),
        P("tp"),
        P("tp"),
        P("tp"),
        P("tp"),
        P("tp", None),
        P("tp", None),
        P(),
        P(),
        P(SEQ, "tp"),
        P(SEQ, "tp"),
        P(SEQ, "tp"),
        P(),
    )
    inner = 2
    outer = mesh.shape["sp"] // inner
    cut = jax.sharding.Mesh(
        mesh.devices.reshape(outer, inner, mesh.shape["tp"]), (OUTER, INNER, "tp")
    )
    return jax.shard_map(
        layer, mesh=cut, in_specs=placed, out_specs=P((*SEQ, "tp"), None), check_vma=False
    )
```
